32 devices in a mesh: sp: 16 (over z, y, core), tp: 2 (over x).
Axes of the slice: x: 2, y: 2, z: 4, core: 2. Of those that a mesh axis runs over, the one named last changes fastest.
Arguments:
- layer_source_rows: bfloat16 [6144, 2048], P(('sp', 'tp')), may hold values from -6 to 6
- entry_rescale_factor: bfloat16 [2048], replicated, may hold values from 0.099609375 to 1.8984375
- sliding_mixer_entry_matrix: bfloat16 [3, 2048, 1024], P(None, 'sp', 'tp'), may hold values from -0.125 to 0.125
- recurrent_mixer_entry_matrix: bfloat16 [2, 2048, 1024], P(None, 'sp', 'tp'), may hold values from -0.125 to 0.125
- latent_write_read_matrix: bfloat16 [2, 2048, 2048], P(None, 'sp', 'tp'), may hold values from -0.125 to 0.125
- timestep_matrix: bfloat16 [2048, 2, 16], P(None, None, 'tp'), may hold values from -0.125 to 0.125
- sliding_kernel_coefficients: bfloat16 [3, 1024], P(None, 'tp'), may hold values from -3.5 to 3.5
- recurrent_kernel_coefficients: bfloat16 [5, 1024], P(None, 'tp'), may hold values from -0.5 to 0.5
- latent_kernel_coefficients: bfloat16 [5, 2, 2048], P(None, None, 'tp'), may hold values from -0.5 to 0.5
- lane_forgetting_rate: float32 [2, 16], P(None, 'tp'), may hold values from 0 to 1
- spike_forgetting_rate: float32 [6144, 16], P('sp', 'tp'), may hold values from -2 to 0
- lane_rescale_factor: bfloat16 [1024], P('tp'), may hold values from 0.099609375 to 1.8984375
- sliding_mixer_exit_matrix: bfloat16 [1024, 2048], P('tp', 'sp'), may hold values from -0.125 to 0.125
- recurrent_mixer_exit_matrix: bfloat16 [1024, 2048], P('tp', 'sp'), may hold values from -0.125 to 0.125
Outputs:
- mixed_out: bfloat16 [6144, 2048], P(('sp', 'tp'))
The draws below stay inside these ranges and needn't reach their ends.
All inputs are finite; a program needn't handle non-finite values.
Results may differ from the reference program's by a relative error of at most 0.017.
Values may be sent and summed in bfloat16 or wider, within the bound.
No kernel may reach another device: no remote copies, remote signals or barrier semaphores. Data moves between devices by JAX's collectives and lax.ppermute only.
A program may use at most 64 MiB of HBM per device.

```python
import jax
import jax.numpy as jnp
from jax import lax

D = 2048
CONV_CH = 1024
MIXER_LANES = 16
HEAD_DIM = 64
GROUPS = 16
STATE = 128
BLOCK = 128
CONV_TAPS = 3
SSD_TAPS = 5
TOK_DEV = 384
SSD_W = 1024
GROUP_HEADS = 1
SEQ_LENGTH = 6144
N_TP = 2


def draw_lane_forgetting_rate(key, part):
    flag_key = jax.random.fold_in(key, 11)
    level_key = jax.random.fold_in(key, 12)
    fraction = jax.random.uniform(level_key, (2, MIXER_LANES), jnp.float32)
    slow_rates = jnp.exp(jnp.log(0.1 / SEQ_LENGTH) + fraction * jnp.log(5.0))
    fast_rates = jnp.exp(jnp.log(0.01) + fraction * jnp.log(4.0))
    fast_flag = jax.random.randint(flag_key, (2, MIXER_LANES), 0, 2) == 1
    return jnp.where(fast_flag, fast_rates, slow_rates).astype(jnp.float32)


def draw_spike_forgetting_rate(key, part):
    level_key = jax.random.fold_in(key, 21)
    where_random_seed = jax.random.fold_in(key, 22)
    amount_random_seed = jax.random.fold_in(key, 23)
    blocks = SEQ_LENGTH // TOK_DEV
    fraction = jax.random.uniform(level_key, (blocks, MIXER_LANES), jnp.float32)
    levels = jnp.exp(jnp.log(0.1 / SEQ_LENGTH) + fraction * jnp.log(10.0))
    spread_amounts = jnp.repeat(levels, TOK_DEV, axis=0)
    spike_sites = jax.random.randint(where_random_seed, (3, MIXER_LANES), 0, SEQ_LENGTH)
    spike_amounts = jax.random.uniform(amount_random_seed, (3, MIXER_LANES), jnp.float32, 0.22, 0.5)
    sequence_indices = jnp.arange(SEQ_LENGTH)[:, None, None]
    spike_counts = (sequence_indices == spike_sites[None]).astype(jnp.float32)
    return (-spread_amounts - jnp.sum(spike_counts * spike_amounts[None], axis=1)).astype(jnp.float32)


def level_of(key, shape, pieces, least, high):
    loudness, own = 1.0, jax.random.fold_in(key, 6)
    for dim, shards_of in pieces:
        draws = jnp.exp(jax.random.uniform(jax.random.fold_in(own, dim), (shards_of,), jnp.float32, least / len(pieces), high / len(pieces)))
        loudness = loudness * jnp.repeat(draws, shape[dim] // shards_of).reshape([-1 if axis == dim else 1 for axis in range(len(shape))])
    return loudness


def gaussian(own_key, extent, deviation, reach, shards=(), kind=jnp.bfloat16):
    values = deviation * jax.random.normal(own_key, extent, jnp.float32)
    if shards:
        values = values * level_of(own_key, extent, shards, -0.22, 0.18)
    return jnp.clip(values, -reach, reach).astype(kind)


def setup_inputs(seed: int = 0) -> dict:
    streams_of = jax.random.split(jax.random.key(seed), 15)
    layer_source_rows = gaussian(streams_of[0], (SEQ_LENGTH, D), 1.0, 6.0, ((0, 32),))
    entry_rescale_factor = jnp.clip(1.0 + 0.18 * jax.random.normal(streams_of[1], (D,), jnp.float32), 0.099609375, 1.8984375).astype(jnp.bfloat16)
    sliding_mixer_entry_matrix = gaussian(streams_of[2], (3, D, CONV_CH), D ** -0.5, 0.125, ((1, 16), (2, 2)))
    recurrent_mixer_entry_matrix = gaussian(streams_of[3], (2, D, SSD_W), D ** -0.5, 0.125, ((1, 16), (2, 2)))
    latent_write_read_matrix = gaussian(streams_of[4], (2, D, GROUPS * STATE), D ** -0.5, 0.125, ((1, 16), (2, 2)))
    timestep_matrix = gaussian(streams_of[5], (D, 2, MIXER_LANES), D ** -0.5, 0.125, ((2, 2),))
    sliding_kernel_coefficients = gaussian(streams_of[6], (CONV_TAPS, CONV_CH), CONV_TAPS ** -0.5, 3.5, ((1, 2),))
    recurrent_kernel_coefficients = gaussian(streams_of[7], (SSD_TAPS, SSD_W), 0.09, 0.5, ((1, 2),))
    latent_kernel_coefficients = gaussian(streams_of[8], (SSD_TAPS, 2, GROUPS * STATE), 0.09, 0.5, ((2, 2),))
    lane_forgetting_rate = draw_lane_forgetting_rate(jax.random.fold_in(streams_of[14], 71), 0)
    spike_forgetting_rate = draw_spike_forgetting_rate(jax.random.fold_in(streams_of[14], 71), 0)
    lane_rescale_factor = jnp.clip(1.0 + 0.18 * jax.random.normal(streams_of[11], (SSD_W,), jnp.float32), 0.099609375, 1.8984375).astype(jnp.bfloat16)
    sliding_mixer_exit_matrix = gaussian(streams_of[12], (CONV_CH, D), (CONV_CH + SSD_W) ** -0.5, 0.125, ((0, 2), (1, 16)))
    recurrent_mixer_exit_matrix = gaussian(streams_of[13], (SSD_W, D), (CONV_CH + SSD_W) ** -0.5, 0.125, ((0, 2), (1, 16)))
    return dict(layer_source_rows=layer_source_rows, entry_rescale_factor=entry_rescale_factor, sliding_mixer_entry_matrix=sliding_mixer_entry_matrix, recurrent_mixer_entry_matrix=recurrent_mixer_entry_matrix, latent_write_read_matrix=latent_write_read_matrix, timestep_matrix=timestep_matrix, sliding_kernel_coefficients=sliding_kernel_coefficients, recurrent_kernel_coefficients=recurrent_kernel_coefficients, latent_kernel_coefficients=latent_kernel_coefficients, lane_forgetting_rate=lane_forgetting_rate, spike_forgetting_rate=spike_forgetting_rate, lane_rescale_factor=lane_rescale_factor, sliding_mixer_exit_matrix=sliding_mixer_exit_matrix, recurrent_mixer_exit_matrix=recurrent_mixer_exit_matrix)


epsilon = 1e-05

def centred_taps(values, tap_table):
    tap_count = tap_table.shape[0]
    half_width = tap_count // 2
    length = values.shape[0]
    padded = jnp.pad(values, ((half_width, half_width), (0, 0)))
    summed = jnp.zeros(values.shape, jnp.float32)
    for offset in range(tap_count):
        summed = summed + padded[offset:offset + length] * tap_table[offset].astype(jnp.float32)
    return summed

def project(normed, weight):
    return jnp.dot(normed, weight, preferred_element_type=jnp.float32).astype(jnp.bfloat16)

def direction_pass(ssd_x, keys_b, reads_c, timestep_deltas, forgetting_exponent):
    length = ssd_x.shape[0]
    blocks = length // BLOCK
    x_blocks = ssd_x.reshape(blocks, BLOCK, GROUPS, GROUP_HEADS, HEAD_DIM)
    b_blocks = keys_b.reshape(blocks, BLOCK, GROUPS, STATE)
    c_blocks = reads_c.reshape(blocks, BLOCK, GROUPS, STATE)
    d_blocks = timestep_deltas.reshape(blocks, BLOCK, GROUPS, GROUP_HEADS)
    l_blocks = forgetting_exponent.reshape(blocks, BLOCK, GROUPS, GROUP_HEADS)
    lower_mask = (jnp.arange(BLOCK)[:, None] >= jnp.arange(BLOCK)[None, :])[:, :, None, None]

    def one_block(carry_state, inputs):
        x_block, b_block, c_block, d_block, l_block = inputs
        running = jnp.cumsum(l_block, axis=0)
        log_gaps = jnp.where(lower_mask, running[:, None] - running[None, :], 0.0)
        decays = jnp.where(lower_mask, jnp.exp(log_gaps), 0.0)
        scores = jnp.einsum('tgn,sgn->tsg', c_block.astype(jnp.float32), b_block.astype(jnp.float32))
        weights = (scores[..., None] * decays * d_block[None]).astype(jnp.bfloat16)
        within = jnp.einsum('tsgr,sgrp->tgrp', weights.astype(jnp.float32), x_block.astype(jnp.float32))
        entering = lax.optimization_barrier(carry_state.astype(jnp.bfloat16)).astype(jnp.float32)
        carried = jnp.einsum('tgn,grpn->tgrp', c_block.astype(jnp.float32), entering) * jnp.exp(running)[..., None]
        to_end = jnp.exp(running[-1][None] - running) * d_block
        weighted = (x_block.astype(jnp.float32) * to_end[..., None]).astype(jnp.bfloat16)
        contribution = jnp.einsum('sgrp,sgn->grpn', weighted.astype(jnp.float32), b_block.astype(jnp.float32))
        next_state = carry_state * jnp.exp(running[-1])[..., None, None] + contribution
        return (next_state, within + carried)
    initial = jnp.zeros((GROUPS, GROUP_HEADS, HEAD_DIM, STATE), jnp.float32)
    final_state, outputs = lax.scan(one_block, initial, (x_blocks, b_blocks, c_blocks, d_blocks, l_blocks))
    return outputs.reshape(length, GROUPS, GROUP_HEADS, HEAD_DIM)

def reference(layer_source_rows, entry_rescale_factor, sliding_mixer_entry_matrix, recurrent_mixer_entry_matrix, latent_write_read_matrix, timestep_matrix, sliding_kernel_coefficients, recurrent_kernel_coefficients, latent_kernel_coefficients, lane_forgetting_rate, spike_forgetting_rate, lane_rescale_factor, sliding_mixer_exit_matrix, recurrent_mixer_exit_matrix):
    float_rows = layer_source_rows.astype(jnp.float32)
    normed = (float_rows * lax.rsqrt(lax.optimization_barrier(jnp.mean(float_rows * float_rows, axis=-1, keepdims=True)) + epsilon) * entry_rescale_factor.astype(jnp.float32)).astype(jnp.bfloat16)
    out_gate = project(normed, sliding_mixer_entry_matrix[0])
    in_gate = project(normed, sliding_mixer_entry_matrix[1])
    values = project(normed, sliding_mixer_entry_matrix[2])
    ssd_gate = project(normed, recurrent_mixer_entry_matrix[0])
    ssd_in = project(normed, recurrent_mixer_entry_matrix[1])
    inject = project(normed, latent_write_read_matrix[0])
    readout = project(normed, latent_write_read_matrix[1])
    raw_step = project(normed, timestep_matrix.reshape(timestep_matrix.shape[0], 2 * MIXER_LANES)).reshape(-1, 2, MIXER_LANES)
    gated_in = (in_gate.astype(jnp.float32) * values.astype(jnp.float32)).astype(jnp.bfloat16)
    y_conv = (out_gate.astype(jnp.float32) * centred_taps(gated_in.astype(jnp.float32), sliding_kernel_coefficients)).astype(jnp.bfloat16)
    joined = jnp.concatenate([ssd_in, inject, readout], axis=1).astype(jnp.float32)
    joined_taps = jnp.concatenate([recurrent_kernel_coefficients, latent_kernel_coefficients.reshape(latent_kernel_coefficients.shape[0], -1)], axis=1)
    mixed_ssd = jax.nn.silu(centred_taps(joined, joined_taps)).astype(jnp.bfloat16)
    length = layer_source_rows.shape[0]
    ssd_x = mixed_ssd[:, :SSD_W]
    keys_b = mixed_ssd[:, SSD_W:SSD_W + GROUPS * STATE]
    reads_c = mixed_ssd[:, SSD_W + GROUPS * STATE:]
    timestep_deltas = jax.nn.softplus(raw_step.astype(jnp.float32))
    forgetting_exponent = -timestep_deltas * lane_forgetting_rate.astype(jnp.float32)[None] + spike_forgetting_rate.astype(jnp.float32)[:, None, :]
    y_fwd = direction_pass(ssd_x, keys_b, reads_c, timestep_deltas[:, 0], forgetting_exponent[:, 0])
    y_bwd = jnp.flip(direction_pass(jnp.flip(ssd_x, 0), jnp.flip(keys_b, 0), jnp.flip(reads_c, 0), jnp.flip(timestep_deltas[:, 1], 0), jnp.flip(forgetting_exponent[:, 1], 0)), 0)
    gated_out = (y_fwd + y_bwd).reshape(length, SSD_W) * jax.nn.silu(ssd_gate.astype(jnp.float32))
    grouped = gated_out.reshape(length, GROUPS, GROUP_HEADS * HEAD_DIM)
    grouped = grouped * lax.rsqrt(lax.optimization_barrier(jnp.mean(grouped * grouped, axis=-1, keepdims=True)) + epsilon)
    y_ssd = (grouped.reshape(length, SSD_W) * lane_rescale_factor.astype(jnp.float32)).astype(jnp.bfloat16)
    conv_part = CONV_CH // N_TP
    ssd_part = SSD_W // N_TP
    summed = jnp.zeros((length, D), jnp.float32)
    for source in range(N_TP):
        partial_value = jnp.dot(y_conv[:, source * conv_part:(source + 1) * conv_part], sliding_mixer_exit_matrix[source * conv_part:(source + 1) * conv_part], preferred_element_type=jnp.float32)
        partial_value = partial_value + jnp.dot(y_ssd[:, source * ssd_part:(source + 1) * ssd_part], recurrent_mixer_exit_matrix[source * ssd_part:(source + 1) * ssd_part], preferred_element_type=jnp.float32)
        summed = summed + lax.optimization_barrier(partial_value.astype(jnp.bfloat16)).astype(jnp.float32)
    return summed.astype(jnp.bfloat16)
```

```python
import jax
import jax.numpy as jnp
from jax import lax
from jax.sharding import PartitionSpec as P

HEAD_DIM = 64
STATE = 128
BLOCK = 128
HALO = 8


epsilon = 1e-05


def swapped(value, axis, distance):
    size = lax.axis_size(axis)
    return lax.ppermute(value, axis, [(i, i ^ distance) for i in range(size)])


def tp_rows(normed):
    if lax.axis_size("tp") != 2:
        return lax.all_gather(normed, "tp", axis=0, tiled=True)
    mine = lax.axis_index("tp")
    count = normed.shape[0]
    other = swapped(normed, "tp", 1)
    rows = jnp.zeros((2 * count, normed.shape[1]), normed.dtype)
    rows = lax.dynamic_update_slice(rows, normed, (mine * count, 0))
    return lax.dynamic_update_slice(rows, other, ((1 - mine) * count, 0))


def with_halo(rows):
    size = lax.axis_size("sp")
    up = [(i, i + 1) for i in range(size - 1)]
    down = [(i + 1, i) for i in range(size - 1)]
    before = lax.ppermute(rows[-HALO:], "sp", up)
    after = lax.ppermute(rows[:HALO], "sp", down)
    return jnp.concatenate([before, rows, after], axis=0)


def apply_taps(padded, tap_table, length):
    taps = tap_table.shape[0]
    first = HALO - taps // 2
    summed = jnp.zeros((length, padded.shape[1]), jnp.float32)
    for offset in range(taps):
        summed = summed + padded[first + offset : first + offset + length].astype(
            jnp.float32
        ) * tap_table[offset].astype(jnp.float32)
    return summed


def decay_levels(decay):
    place = lax.axis_index("sp")
    levels = []
    ahead = jnp.ones_like(decay)
    distance = 1
    while distance < lax.axis_size("sp"):
        other = swapped(decay, "sp", distance)
        upper = (place & distance) != 0
        joins = jnp.stack([upper, ~upper])
        levels.append((distance, joins[:, None], decay, other, ahead))
        ahead = jnp.where(joins[:, None], ahead * other, ahead)
        decay = decay * other
        distance *= 2
    return levels


def entering_state(total, levels):
    place = lax.axis_index("sp")
    prefix = jnp.zeros_like(total)
    for number, (distance, joins, own, other, ahead) in enumerate(levels):
        wide = lambda a: a[..., None, None]
        joins = joins[None, :, :, None]
        if number + 1 < len(levels):
            got = swapped(total.astype(jnp.bfloat16), "sp", distance).astype(jnp.float32)
            prefix = jnp.where(joins, got * wide(ahead) + prefix, prefix)
            total = jnp.where(joins, got * wide(own) + total, total * wide(other) + got)
        else:
            upper = (place & distance) != 0
            send = jnp.where(upper, total[:, 1], total[:, 0]).astype(jnp.bfloat16)
            got = swapped(send, "sp", distance).astype(jnp.float32)
            prefix = jnp.where(joins, got[:, None] * wide(ahead) + prefix, prefix)
    return prefix


def local(
    layer_source_rows,
    entry_rescale_factor,
    sliding_mixer_entry_matrix,
    recurrent_mixer_entry_matrix,
    latent_write_read_matrix,
    timestep_matrix,
    sliding_kernel_coefficients,
    recurrent_kernel_coefficients,
    latent_kernel_coefficients,
    lane_forgetting_rate,
    spike_forgetting_rate,
    lane_rescale_factor,
    sliding_mixer_exit_matrix,
    recurrent_mixer_exit_matrix,
):
    f32, bf16 = jnp.float32, jnp.bfloat16
    conv_width = sliding_mixer_entry_matrix.shape[2]
    ssd_width = recurrent_mixer_entry_matrix.shape[2]
    state_width = latent_write_read_matrix.shape[2]
    heads = timestep_matrix.shape[2]
    assert state_width == heads * STATE and ssd_width == heads * HEAD_DIM

    ssd_shard = jnp.concatenate(
        [
            recurrent_mixer_entry_matrix[0],
            recurrent_mixer_entry_matrix[1],
            latent_write_read_matrix[0],
            latent_write_read_matrix[1],
        ],
        axis=1,
    )
    ssd_weight = lax.all_gather(ssd_shard, "sp", axis=0, tiled=True)

    float_rows = layer_source_rows.astype(f32)
    normed = (
        float_rows
        * lax.rsqrt(jnp.mean(float_rows * float_rows, axis=-1, keepdims=True) + epsilon)
        * entry_rescale_factor.astype(f32)
    ).astype(bf16)
    rows = tp_rows(normed)
    length = rows.shape[0]

    exit_shard = jnp.concatenate(
        [sliding_mixer_exit_matrix, recurrent_mixer_exit_matrix], axis=0
    ).T
    conv_shard = jnp.concatenate(
        [sliding_mixer_entry_matrix[k] for k in range(3)] + [exit_shard], axis=1
    )
    conv_shard, rows = lax.optimization_barrier((conv_shard, rows))
    conv_weight = lax.all_gather(conv_shard, "sp", axis=0, tiled=True)

    wide_rows = with_halo(rows)

    raw_step = (
        jnp.dot(rows, timestep_matrix.reshape(-1, 2 * heads), preferred_element_type=f32)
        .astype(bf16)
        .astype(f32)
        .reshape(length, 2, heads)
    )
    deltas = jax.nn.softplus(raw_step)
    log_decay = -deltas * lane_forgetting_rate[None] + spike_forgetting_rate[:, None, :]
    blocks = length // BLOCK
    order = jnp.arange(BLOCK)
    lower = (order[:, None] >= order[None, :]).astype(f32)
    sums = jnp.stack([lower, lower.T])
    logs = log_decay.reshape(blocks, BLOCK, 2, heads).transpose(2, 3, 0, 1)
    delta = deltas.reshape(blocks, BLOCK, 2, heads).transpose(2, 3, 0, 1)
    running = jnp.einsum("dhbs,dts->dhbt", logs, sums, precision=lax.Precision.HIGHEST)
    ends = jnp.stack([running[0, :, :, -1], running[1, :, :, 0]])
    to_end = jnp.exp(ends[..., None] - running) * delta
    levels = decay_levels(jnp.exp(jnp.sum(ends, axis=-1)))
    levels = [(n, j, a.T, b.T, c.T) for n, j, a, b, c in levels]
    before_ends = jnp.cumsum(ends[0], axis=-1) - ends[0]
    after_ends = jnp.cumsum(ends[1][:, ::-1], axis=-1)[:, ::-1] - ends[1]
    starts = jnp.exp(jnp.stack([before_ends, after_ends]))
    mask = order[:, None] >= order[None, :]
    gaps = running[..., :, None] - running[..., None, :]
    decays = (
        jnp.where(mask, jnp.exp(jnp.where(mask, gaps[0], 0.0)), 0.0) * delta[0][..., None, :]
        + jnp.where(mask.T, jnp.exp(jnp.where(mask.T, gaps[1], 0.0)), 0.0)
        * delta[1][..., None, :]
    )

    projected = jnp.dot(wide_rows, ssd_weight, preferred_element_type=f32).astype(bf16)
    ssd_gate = projected[HALO : HALO + length, :ssd_width]
    joined_taps = jnp.concatenate(
        [
            recurrent_kernel_coefficients,
            latent_kernel_coefficients.reshape(latent_kernel_coefficients.shape[0], -1),
        ],
        axis=1,
    )
    mixed = jax.nn.silu(apply_taps(projected[:, ssd_width:], joined_taps, length)).astype(bf16)
    ssd_x = mixed[:, :ssd_width].reshape(blocks, BLOCK, heads, HEAD_DIM)
    keys_b = mixed[:, ssd_width : ssd_width + state_width].reshape(blocks, BLOCK, heads, STATE)
    reads_c = mixed[:, ssd_width + state_width :].reshape(blocks, BLOCK, heads, STATE)
    ssd_x = ssd_x.transpose(2, 0, 1, 3)
    keys_b = keys_b.transpose(2, 0, 1, 3)
    reads_c = reads_c.transpose(2, 0, 1, 3)

    x_float = ssd_x.astype(f32)
    weighted = jnp.concatenate(
        [(x_float * to_end[d][..., None]).astype(bf16) for d in range(2)], axis=-1
    )
    contribution = jnp.einsum("hbsp,hbsn->hbpn", weighted, keys_b, preferred_element_type=f32)
    contribution = contribution.reshape(heads, blocks, 2, HEAD_DIM, STATE)
    end_decay = jnp.exp(ends)[..., None, None]
    forward, fore = [], jnp.zeros((heads, HEAD_DIM, STATE), f32)
    for b in range(blocks):
        forward.append(fore)
        fore = fore * end_decay[0, :, b] + contribution[:, b, 0]
    backward, aft = [None] * blocks, jnp.zeros((heads, HEAD_DIM, STATE), f32)
    for b in reversed(range(blocks)):
        backward[b] = aft
        aft = aft * end_decay[1, :, b] + contribution[:, b, 1]
    prefix = entering_state(jnp.stack([fore, aft], axis=1), levels)

    scores = jnp.einsum("hbtn,hbsn->hbts", reads_c, keys_b, preferred_element_type=f32)
    within = jnp.einsum(
        "hbts,hbsp->hbtp", (scores * decays).astype(bf16), ssd_x, preferred_element_type=f32
    )
    inside = jnp.stack([jnp.stack(forward, 1), jnp.stack(backward, 1)], axis=2)
    entering = inside + prefix[:, None] * starts.transpose(1, 2, 0)[..., None, None]
    entering = entering.astype(bf16).reshape(heads, blocks, 2 * HEAD_DIM, STATE)
    carried = jnp.einsum("hbtn,hbpn->hbtp", reads_c, entering, preferred_element_type=f32)
    grown = jnp.exp(running)[..., None]
    y = within + carried[..., :HEAD_DIM] * grown[0] + carried[..., HEAD_DIM:] * grown[1]
    gate = ssd_gate.astype(f32).reshape(blocks, BLOCK, heads, HEAD_DIM).transpose(2, 0, 1, 3)
    y = y * jax.nn.silu(gate)
    y = y * lax.rsqrt(jnp.mean(y * y, axis=-1, keepdims=True) + epsilon)
    y = y * lane_rescale_factor.astype(f32).reshape(heads, 1, 1, HEAD_DIM)
    y_ssd = y.astype(bf16).transpose(1, 2, 0, 3).reshape(length, ssd_width)

    conv = jnp.dot(
        wide_rows, conv_weight[:, : 3 * conv_width], preferred_element_type=f32
    ).astype(bf16)
    out_gate = conv[HALO : HALO + length, :conv_width].astype(f32)
    gated_in = (
        conv[:, conv_width : 2 * conv_width].astype(f32) * conv[:, 2 * conv_width :].astype(f32)
    ).astype(bf16)
    y_conv = (out_gate * apply_taps(gated_in, sliding_kernel_coefficients, length)).astype(bf16)

    mixed_y = jnp.concatenate([y_conv, y_ssd], axis=1)
    exit_weight = conv_weight[:, 3 * conv_width :]

    def leave(part):
        return lax.dot_general(
            part, exit_weight, (((1,), (1,)), ((), ())), preferred_element_type=f32
        ).astype(bf16)

    if lax.axis_size("tp") != 2:
        return lax.psum_scatter(leave(mixed_y), "tp", scatter_dimension=0, tiled=True)
    mine = lax.axis_index("tp")
    half = length // 2
    sent = leave(lax.dynamic_slice_in_dim(mixed_y, (1 - mine) * half, half, 0))
    got = swapped(sent, "tp", 1)
    kept = leave(lax.dynamic_slice_in_dim(mixed_y, mine * half, half, 0))
    return (kept.astype(f32) + got.astype(f32)).astype(bf16)


def solution(mesh):
    placed = (
        P(("sp", "tp"), None),
        P(),
        P(None, "sp", "tp"),
        P(None, "sp", "tp"),
        P(None, "sp", "tp"),
        P(None, None, "tp"),
        P(None, "tp"),
        P(None, "tp"),
        P(None, None, "tp"),
        P(None, "tp"),
        P("sp", "tp"),
        P("tp"),
        P("tp", "sp"),
        P("tp", "sp"),
    )
    return jax.shard_map(
        local, mesh=mesh, in_specs=placed, out_specs=P(("sp", "tp"), None), check_vma=False
    )
```

```python
import jax
import jax.numpy as jnp
from jax import lax
from jax.sharding import PartitionSpec as P

HEAD_DIM = 64
STATE = 128
BLOCK = 128
HALO = 8


epsilon = 1e-05


def swapped(value, axis, distance):
    size = lax.axis_size(axis)
    return lax.ppermute(value, axis, [(i, i ^ distance) for i in range(size)])


def tp_rows(normed):
    if lax.axis_size("tp") != 2:
        return lax.all_gather(normed, "tp", axis=0, tiled=True)
    mine = lax.axis_index("tp")
    count = normed.shape[0]
    other = swapped(normed, "tp", 1)
    rows = jnp.zeros((2 * count, normed.shape[1]), normed.dtype)
    rows = lax.dynamic_update_slice(rows, normed, (mine * count, 0))
    return lax.dynamic_update_slice(rows, other, ((1 - mine) * count, 0))


def with_halo(rows):
    size = lax.axis_size("sp")
    up = [(i, i + 1) for i in range(size - 1)]
    down = [(i + 1, i) for i in range(size - 1)]
    before = lax.ppermute(rows[-HALO:], "sp", up)
    after = lax.ppermute(rows[:HALO], "sp", down)
    return jnp.concatenate([before, rows, after], axis=0)


def shifted(value, distance):
    size = lax.axis_size("sp")
    return lax.ppermute(value, "sp", [(i, (i + distance) % size) for i in range(size)])


def ring_ready():
    return lax.axis_size("sp") == 16


def gathered_pair(shard, after=None):
    if after is not None:
        shard, _ = lax.optimization_barrier((shard, after))
    side = swapped(shard, "sp", 2)
    low = shifted(shard, 4)
    high = shifted(shard, -4)
    far = shifted(low, 4)
    side_low = swapped(low, "sp", 2)
    side_high = shifted(side, -4)
    half = shard.shape[0] // 2
    side_far = [shifted(side_low[:half], 4), shifted(side_high[half:], -4)]
    own = jnp.concatenate([shard, side, low, high, far, side_low, side_high] + side_far, axis=0)
    return own, swapped(own, "sp", 1), side


def pair_sources():
    size, place = lax.axis_size("sp"), lax.axis_index("sp")
    across = place ^ 2
    return [
        where % size
        for where in (
            place,
            across,
            place - 4 + size,
            place + 4,
            place - 8 + size,
            across - 4 + size,
            across + 4,
            across + 8,
        )
    ]


def picked(rows, sources):
    width = rows.shape[1] // lax.axis_size("sp")
    return jnp.concatenate(
        [lax.dynamic_slice_in_dim(rows, where * width, width, 1) for where in sources], axis=1
    )


def apply_taps(padded, tap_table, length):
    taps = tap_table.shape[0]
    first = HALO - taps // 2
    summed = jnp.zeros((length, padded.shape[1]), jnp.float32)
    for offset in range(taps):
        summed = summed + padded[first + offset : first + offset + length].astype(
            jnp.float32
        ) * tap_table[offset].astype(jnp.float32)
    return summed


def decay_levels(decay):
    place = lax.axis_index("sp")
    levels = []
    ahead = jnp.ones_like(decay)
    distance = 1
    while distance < lax.axis_size("sp"):
        other = swapped(decay, "sp", distance)
        upper = (place & distance) != 0
        joins = jnp.stack([upper, ~upper])
        levels.append((distance, joins[:, None], decay, other, ahead))
        ahead = jnp.where(joins[:, None], ahead * other, ahead)
        decay = decay * other
        distance *= 2
    return levels


def entering_state(total, levels):
    place = lax.axis_index("sp")
    prefix = jnp.zeros_like(total)
    for number, (distance, joins, own, other, ahead) in enumerate(levels):
        wide = lambda a: a[..., None, None]
        joins = joins[None, :, :, None]
        if number + 1 < len(levels):
            got = swapped(total.astype(jnp.bfloat16), "sp", distance).astype(jnp.float32)
            prefix = jnp.where(joins, got * wide(ahead) + prefix, prefix)
            total = jnp.where(joins, got * wide(own) + total, total * wide(other) + got)
        else:
            upper = (place & distance) != 0
            send = jnp.where(upper, total[:, 1], total[:, 0]).astype(jnp.bfloat16)
            got = swapped(send, "sp", distance).astype(jnp.float32)
            prefix = jnp.where(joins, got[:, None] * wide(ahead) + prefix, prefix)
    return prefix


def local(
    layer_source_rows,
    entry_rescale_factor,
    sliding_mixer_entry_matrix,
    recurrent_mixer_entry_matrix,
    latent_write_read_matrix,
    timestep_matrix,
    sliding_kernel_coefficients,
    recurrent_kernel_coefficients,
    latent_kernel_coefficients,
    lane_forgetting_rate,
    spike_forgetting_rate,
    lane_rescale_factor,
    sliding_mixer_exit_matrix,
    recurrent_mixer_exit_matrix,
):
    f32, bf16 = jnp.float32, jnp.bfloat16
    conv_width = sliding_mixer_entry_matrix.shape[2]
    ssd_width = recurrent_mixer_entry_matrix.shape[2]
    state_width = latent_write_read_matrix.shape[2]
    heads = timestep_matrix.shape[2]
    assert state_width == heads * STATE and ssd_width == heads * HEAD_DIM

    ssd_shard = jnp.concatenate(
        [
            recurrent_mixer_entry_matrix[0],
            recurrent_mixer_entry_matrix[1],
            latent_write_read_matrix[0],
            latent_write_read_matrix[1],
        ],
        axis=1,
    )
    ring = ring_ready()
    if ring:
        ssd_own, ssd_other, token = gathered_pair(ssd_shard)
    else:
        ssd_weight = lax.all_gather(ssd_shard, "sp", axis=0, tiled=True)

    float_rows = layer_source_rows.astype(f32)
    normed = (
        float_rows
        * lax.rsqrt(jnp.mean(float_rows * float_rows, axis=-1, keepdims=True) + epsilon)
        * entry_rescale_factor.astype(f32)
    ).astype(bf16)
    rows = tp_rows(normed)
    length = rows.shape[0]

    exit_shard = jnp.concatenate(
        [sliding_mixer_exit_matrix, recurrent_mixer_exit_matrix], axis=0
    ).T
    conv_shard = jnp.concatenate([sliding_mixer_entry_matrix[k] for k in range(3)], axis=1)
    exit_weight = lax.all_gather(exit_shard, "sp", axis=0, tiled=True)
    if ring:
        conv_own, conv_other, _ = gathered_pair(conv_shard, token)
    else:
        conv_weight = lax.all_gather(conv_shard, "sp", axis=0, tiled=True)

    wide_rows = with_halo(rows)
    if ring:
        sources = pair_sources()
        rows_own = picked(wide_rows, sources)
        rows_other = picked(wide_rows, [where ^ 1 for where in sources])

    raw_step = (
        jnp.dot(rows, timestep_matrix.reshape(-1, 2 * heads), preferred_element_type=f32)
        .astype(bf16)
        .astype(f32)
        .reshape(length, 2, heads)
    )
    deltas = jax.nn.softplus(raw_step)
    log_decay = -deltas * lane_forgetting_rate[None] + spike_forgetting_rate[:, None, :]
    blocks = length // BLOCK
    order = jnp.arange(BLOCK)
    lower = (order[:, None] >= order[None, :]).astype(f32)
    sums = jnp.stack([lower, lower.T])
    logs = log_decay.reshape(blocks, BLOCK, 2, heads).transpose(2, 3, 0, 1)
    delta = deltas.reshape(blocks, BLOCK, 2, heads).transpose(2, 3, 0, 1)
    running = jnp.einsum("dhbs,dts->dhbt", logs, sums, precision=lax.Precision.HIGHEST)
    ends = jnp.stack([running[0, :, :, -1], running[1, :, :, 0]])
    to_end = jnp.exp(ends[..., None] - running) * delta
    levels = decay_levels(jnp.exp(jnp.sum(ends, axis=-1)))
    levels = [(n, j, a.T, b.T, c.T) for n, j, a, b, c in levels]
    before_ends = jnp.cumsum(ends[0], axis=-1) - ends[0]
    after_ends = jnp.cumsum(ends[1][:, ::-1], axis=-1)[:, ::-1] - ends[1]
    starts = jnp.exp(jnp.stack([before_ends, after_ends]))
    mask = order[:, None] >= order[None, :]
    gaps = running[..., :, None] - running[..., None, :]
    decays = (
        jnp.where(mask, jnp.exp(jnp.where(mask, gaps[0], 0.0)), 0.0) * delta[0][..., None, :]
        + jnp.where(mask.T, jnp.exp(jnp.where(mask.T, gaps[1], 0.0)), 0.0)
        * delta[1][..., None, :]
    )

    if ring:
        projected = jnp.dot(rows_own, ssd_own, preferred_element_type=f32)
        projected = projected + jnp.dot(rows_other, ssd_other, preferred_element_type=f32)
        projected = projected.astype(bf16)
    else:
        projected = jnp.dot(wide_rows, ssd_weight, preferred_element_type=f32).astype(bf16)
    ssd_gate = projected[HALO : HALO + length, :ssd_width]
    joined_taps = jnp.concatenate(
        [
            recurrent_kernel_coefficients,
            latent_kernel_coefficients.reshape(latent_kernel_coefficients.shape[0], -1),
        ],
        axis=1,
    )
    mixed = jax.nn.silu(apply_taps(projected[:, ssd_width:], joined_taps, length)).astype(bf16)
    ssd_x = mixed[:, :ssd_width].reshape(blocks, BLOCK, heads, HEAD_DIM)
    keys_b = mixed[:, ssd_width : ssd_width + state_width].reshape(blocks, BLOCK, heads, STATE)
    reads_c = mixed[:, ssd_width + state_width :].reshape(blocks, BLOCK, heads, STATE)
    ssd_x = ssd_x.transpose(2, 0, 1, 3)
    keys_b = keys_b.transpose(2, 0, 1, 3)
    reads_c = reads_c.transpose(2, 0, 1, 3)

    x_float = ssd_x.astype(f32)
    weighted = jnp.concatenate(
        [(x_float * to_end[d][..., None]).astype(bf16) for d in range(2)], axis=-1
    )
    contribution = jnp.einsum("hbsp,hbsn->hbpn", weighted, keys_b, preferred_element_type=f32)
    contribution = contribution.reshape(heads, blocks, 2, HEAD_DIM, STATE)
    end_decay = jnp.exp(ends)[..., None, None]
    forward, fore = [], jnp.zeros((heads, HEAD_DIM, STATE), f32)
    for b in range(blocks):
        forward.append(fore)
        fore = fore * end_decay[0, :, b] + contribution[:, b, 0]
    backward, aft = [None] * blocks, jnp.zeros((heads, HEAD_DIM, STATE), f32)
    for b in reversed(range(blocks)):
        backward[b] = aft
        aft = aft * end_decay[1, :, b] + contribution[:, b, 1]
    prefix = entering_state(jnp.stack([fore, aft], axis=1), levels)

    scores = jnp.einsum("hbtn,hbsn->hbts", reads_c, keys_b, preferred_element_type=f32)
    within = jnp.einsum(
        "hbts,hbsp->hbtp", (scores * decays).astype(bf16), ssd_x, preferred_element_type=f32
    )
    inside = jnp.stack([jnp.stack(forward, 1), jnp.stack(backward, 1)], axis=2)
    entering = inside + prefix[:, None] * starts.transpose(1, 2, 0)[..., None, None]
    entering = entering.astype(bf16).reshape(heads, blocks, 2 * HEAD_DIM, STATE)
    carried = jnp.einsum("hbtn,hbpn->hbtp", reads_c, entering, preferred_element_type=f32)
    grown = jnp.exp(running)[..., None]
    y = within + carried[..., :HEAD_DIM] * grown[0] + carried[..., HEAD_DIM:] * grown[1]
    gate = ssd_gate.astype(f32).reshape(blocks, BLOCK, heads, HEAD_DIM).transpose(2, 0, 1, 3)
    y = y * jax.nn.silu(gate)
    y = y * lax.rsqrt(jnp.mean(y * y, axis=-1, keepdims=True) + epsilon)
    y = y * lane_rescale_factor.astype(f32).reshape(heads, 1, 1, HEAD_DIM)
    y_ssd = y.astype(bf16).transpose(1, 2, 0, 3).reshape(length, ssd_width)

    if ring:
        conv = jnp.dot(rows_own, conv_own, preferred_element_type=f32)
        conv = conv + jnp.dot(rows_other, conv_other, preferred_element_type=f32)
        conv = conv.astype(bf16)
    else:
        conv = jnp.dot(wide_rows, conv_weight, preferred_element_type=f32).astype(bf16)
    out_gate = conv[HALO : HALO + length, :conv_width].astype(f32)
    gated_in = (
        conv[:, conv_width : 2 * conv_width].astype(f32) * conv[:, 2 * conv_width :].astype(f32)
    ).astype(bf16)
    y_conv = (out_gate * apply_taps(gated_in, sliding_kernel_coefficients, length)).astype(bf16)

    mixed_y = jnp.concatenate([y_conv, y_ssd], axis=1)

    def leave(part):
        return lax.dot_general(
            part, exit_weight, (((1,), (1,)), ((), ())), preferred_element_type=f32
        ).astype(bf16)

    if lax.axis_size("tp") != 2:
        return lax.psum_scatter(leave(mixed_y), "tp", scatter_dimension=0, tiled=True)
    mine = lax.axis_index("tp")
    half = length // 2
    sent = leave(lax.dynamic_slice_in_dim(mixed_y, (1 - mine) * half, half, 0))
    got = swapped(sent, "tp", 1)
    kept = leave(lax.dynamic_slice_in_dim(mixed_y, mine * half, half, 0))
    return (kept.astype(f32) + got.astype(f32)).astype(bf16)


def solution(mesh):
    placed = (
        P(("sp", "tp"), None),
        P(),
        P(None, "sp", "tp"),
        P(None, "sp", "tp"),
        P(None, "sp", "tp"),
        P(None, None, "tp"),
        P(None, "tp"),
        P(None, "tp"),
        P(None, None, "tp"),
        P(None, "tp"),
        P("sp", "tp"),
        P("tp"),
        P("tp", "sp"),
        P("tp", "sp"),
    )
    return jax.shard_map(
        local, mesh=mesh, in_specs=placed, out_specs=P(("sp", "tp"), None), check_vma=False
    )
```
